256 devices in a mesh: sp: 32 (over z, x), tp: 8 (over y, core).
Axes of the slice: x: 4, y: 4, z: 8, core: 2. Of those that a mesh axis runs over, the one named last changes fastest.
Arguments:
- residual: bfloat16 [24576, 2048], P('sp'), may hold values from -6 to 6
- query_matrix: bfloat16 [24576, 1024], P('sp', 'tp'), may hold values from -6 to 6
- key_matrix: bfloat16 [24576, 1024], P('sp', 'tp'), may hold values from -6 to 6
- value_matrix: bfloat16 [24576, 2048], P('sp', 'tp'), may hold values from -6 to 6
- output_gate_logit: bfloat16 [24576, 2048], P('sp', 'tp'), may hold values from -6 to 6
- input_gate_log: float32 [24576, 8], P('sp', 'tp'), may hold values from -4 to 125
- forget_gate_logit: float32 [24576, 8], P('sp', 'tp')
- extra_head_decay: float32 [24576, 8], P('sp', 'tp'), may hold values from -1 to 0
- head_norm_gain: float32 [2048], P('tp'), may hold values from 0.1 to 1.9
- projection: bfloat16 [2048, 2048], P('tp'), may hold values from -5.303301 to 5.303301
- cell_output_gain: float32 [2048], replicated, may hold values from 0.1 to 1.9
- mixer_input_gain: float32 [2048], replicated, may hold values from 0.1 to 1.9
- mixer_gate_weight: bfloat16 [2048, 5120], P('sp', 'tp'), may hold values from -0.125 to 0.125
- mixer_up_weight: bfloat16 [2048, 5120], P('sp', 'tp'), may hold values from -0.125 to 0.125
- mixer_down_weight: bfloat16 [5120, 2048], P('tp', 'sp'), may hold values from -0.078125 to 0.078125
Outputs:
- updated: bfloat16 [24576, 2048], P('sp', 'tp')
The draws below stay inside these ranges and needn't reach their ends.
All inputs are finite; a program needn't handle non-finite values.
Results may differ from the reference program's by a relative error of at most 0.014.
Values may be sent and summed in bfloat16 or wider, within the bound.
A program may use at most 128 MiB of HBM per device.

```python
import math
import jax
import jax.numpy as jnp
from jax import lax

D = 2048
HEADS = 8
DQK = 128
DV = 256
FF = 5120
TOK_DEV = 768
TOKENS = 24576
M_V = 2048
N_TP = 8


def draw_input_gate_log(key, part):
    values = jnp.clip(jax.random.normal(key, (TOKENS, HEADS), jnp.float32), -4.0, 4.0)
    return values


def draw_forget_gate_logit(key, part):
    slow_limit = 5
    slow = jax.random.randint(jax.random.fold_in(key, 1), (HEADS,), 0, 10) < slow_limit
    quick = jnp.log(jax.random.uniform(jax.random.fold_in(key, 2), (HEADS,), jnp.float32, 30.0, 60.0))
    level = jnp.where(slow, jnp.log(4.0 * TOKENS), quick)
    shifts = jax.random.uniform(jax.random.fold_in(key, 3), (TOKENS // TOK_DEV, HEADS), jnp.float32, -0.7, 0.7)
    shifts = jnp.repeat(shifts, TOK_DEV, axis=0)
    noise = jnp.clip(jax.random.normal(jax.random.fold_in(key, 4), (TOKENS, HEADS), jnp.float32), -4.0, 4.0)
    return level[None, :] + shifts + noise


def draw_extra_head_decay(key, part):
    spots = jax.random.randint(jax.random.fold_in(key, 1), (3, HEADS), 0, TOKENS)
    depth = jnp.log(jax.random.uniform(jax.random.fold_in(key, 2), (3, HEADS), jnp.float32, 0.5, 0.8))
    columns = lax.broadcasted_iota(jnp.int32, (3, HEADS), 1)
    return jnp.zeros((TOKENS, HEADS), jnp.float32).at[spots, columns].set(depth)


def draw_projection(key, part):
    base = jnp.clip(jax.random.normal(key, (M_V, D), jnp.float32), -6.0, 6.0) * M_V ** (-0.5)
    position = lax.broadcasted_iota(jnp.float32, (1, D), 1) / D
    jitter = jnp.exp(jax.random.uniform(jax.random.fold_in(key, 3), (1, D), jnp.float32, -0.35, 0.35))
    return (base * jnp.exp(1.0986 * position) * jitter).astype(jnp.bfloat16)


def level_of(rng, extent, shards, smallest, top_value):
    loudness = 1.0
    for axis_at, blocks in shards:
        steps = jax.random.uniform(jax.random.fold_in(jax.random.fold_in(rng, 6), axis_at), (blocks,), jnp.float32, smallest / len(shards), top_value / len(shards))
        loudness = loudness * jnp.repeat(jnp.exp(steps), extent[axis_at] // blocks).reshape((-1,) + (1,) * (len(extent) - 1 - axis_at))
    return loudness


def centred(stream_key, dims, scale, reach, cuts=(), kind=jnp.bfloat16):
    values = jax.random.normal(stream_key, dims, jnp.float32) * scale
    if len(cuts) > 0:
        values = level_of(stream_key, dims, cuts, -0.22, 0.18) * values
    return jnp.clip(values, min=-reach, max=reach).astype(kind)


def setup_inputs(seed: int = 0) -> dict:
    arg_keys = jax.random.split(jax.random.key(seed), 16)
    return {
        "residual": centred(arg_keys[0], (TOKENS, D), 1.0, 6.0, ((0, 32),)),
        "query_matrix": centred(arg_keys[1], (TOKENS, HEADS * DQK), 1.0, 6.0, ((0, 32), (1, 8))),
        "key_matrix": centred(arg_keys[2], (TOKENS, HEADS * DQK), 1.0, 6.0, ((0, 32), (1, 8))),
        "value_matrix": centred(arg_keys[3], (TOKENS, M_V), 1.0, 6.0, ((0, 32), (1, 8))),
        "output_gate_logit": centred(arg_keys[4], (TOKENS, M_V), 1.0, 6.0, ((0, 32), (1, 8))),
        "input_gate_log": draw_input_gate_log(jax.random.fold_in(arg_keys[15], 71), 0),
        "forget_gate_logit": draw_forget_gate_logit(jax.random.fold_in(arg_keys[15], 71), 0),
        "extra_head_decay": draw_extra_head_decay(jax.random.fold_in(arg_keys[15], 71), 0),
        "head_norm_gain": jnp.clip(1.0 + 0.18 * jax.random.normal(arg_keys[8], (M_V,), jnp.float32), 0.1, 1.9),
        "projection": draw_projection(jax.random.fold_in(arg_keys[15], 71), 0),
        "cell_output_gain": jnp.clip(1.0 + 0.18 * jax.random.normal(arg_keys[10], (D,), jnp.float32), 0.1, 1.9),
        "mixer_input_gain": jnp.clip(1.0 + 0.18 * jax.random.normal(arg_keys[11], (D,), jnp.float32), 0.1, 1.9),
        "mixer_gate_weight": centred(arg_keys[12], (D, FF), D ** -0.5, 0.125, ((0, 32), (1, 8))),
        "mixer_up_weight": centred(arg_keys[13], (D, FF), D ** -0.5, 0.125, ((0, 32), (1, 8))),
        "mixer_down_weight": centred(arg_keys[14], (FF, D), FF ** -0.5, 0.078125, ((0, 8), (1, 32))),
    }


HIGHEST = lax.Precision.HIGHEST
EPSILON = 1e-06

def read_out(query, keyed, valued, in_logs, running_log_total, memory, normalizer, stabilizer):
    length = query.shape[1]
    causal = lax.broadcasted_iota(jnp.int32, (length, length), 0) >= lax.broadcasted_iota(jnp.int32, (length, length), 1)
    spread = running_log_total[:, :, None] - running_log_total[:, None, :] + in_logs[:, None, :]
    spread = jnp.where(causal[None], spread, -jnp.inf)
    carried = running_log_total + stabilizer[:, None]
    running = jnp.maximum(carried, lax.optimization_barrier(jnp.max(spread, axis=-1)))
    scores = jnp.einsum('htd,hsd->hts', query, keyed, precision=HIGHEST) * DQK ** (-0.5)
    weights = jnp.exp(spread - running[:, :, None]) * scores
    weight_low = lax.optimization_barrier(weights.astype(jnp.bfloat16)).astype(jnp.float32)
    scaled = jnp.exp(carried - running)
    scaled_query = query * DQK ** (-0.5)
    numerator = jnp.einsum('hts,hsv->htv', weight_low, valued, precision=HIGHEST)
    numerator = numerator + scaled[:, :, None] * jnp.einsum('hvd,htd->htv', memory, scaled_query, precision=HIGHEST)
    denominator = lax.optimization_barrier(jnp.sum(weights, axis=-1)) + scaled * jnp.einsum('hd,htd->ht', normalizer, scaled_query, precision=HIGHEST)
    return numerator / jnp.maximum(jnp.abs(denominator), jnp.exp(-running))[:, :, None]

def fold_state(keyed, valued, in_logs, running_log_total, memory, normalizer, stabilizer):
    last = running_log_total[:, -1]
    lifted = last[:, None] - running_log_total + in_logs
    new_max = jnp.maximum(last + stabilizer, lax.optimization_barrier(jnp.max(lifted, axis=-1)))
    weights = jnp.exp(lifted - new_max[:, None])
    retained = jnp.exp(last + stabilizer - new_max)
    memory = retained[:, None, None] * memory + jnp.einsum('hsv,hsd->hvd', weights[:, :, None] * valued, keyed, precision=HIGHEST)
    normalizer = retained[:, None] * normalizer + jnp.einsum('hs,hsd->hd', weights, keyed, precision=HIGHEST)
    return (memory, normalizer, new_max)

def block_sum(left, right, parts):
    rows = left.shape[0]
    inner = left.shape[1] // parts
    left_blocks = left.reshape(rows, parts, inner).transpose(1, 0, 2)
    right_blocks = right.reshape(parts, inner, right.shape[1])

    def accumulate(total, pair):
        product = jnp.dot(pair[0], pair[1], preferred_element_type=jnp.float32).astype(jnp.bfloat16)
        return (total + lax.optimization_barrier(product).astype(jnp.float32), None)
    total, unused = lax.scan(accumulate, jnp.zeros((rows, right.shape[1]), jnp.float32), (left_blocks, right_blocks))
    return total

def reference(residual, query_matrix, key_matrix, value_matrix, output_gate_logit, input_gate_log, forget_gate_logit, extra_head_decay, head_norm_gain, projection, cell_output_gain, mixer_input_gain, mixer_gate_weight, mixer_up_weight, mixer_down_weight):
    span = math.gcd(TOKENS, 512)
    count = TOKENS // span

    def arrange(array, width):
        return array.astype(jnp.float32).reshape(count, span, HEADS, width).transpose(0, 2, 1, 3)
    query = arrange(query_matrix, DQK)
    keyed = arrange(key_matrix, DQK)
    valued = arrange(value_matrix, DV)
    in_logs = input_gate_log.reshape(count, span, HEADS).transpose(0, 2, 1)
    forget_log_value = jax.nn.log_sigmoid(forget_gate_logit) + extra_head_decay
    running_log_total = jnp.cumsum(forget_log_value.reshape(count, span, HEADS), axis=1).transpose(0, 2, 1)

    def advance(state, blocks):
        memory, normalizer, stabilizer = state
        query_block, key_block, value_block, gate_block, decay_block = blocks
        cells = read_out(query_block, key_block, value_block, gate_block, decay_block, memory, normalizer, stabilizer)
        return (fold_state(key_block, value_block, gate_block, decay_block, memory, normalizer, stabilizer), cells)
    start = (jnp.zeros((HEADS, DV, DQK), jnp.float32), jnp.zeros((HEADS, DQK), jnp.float32), jnp.zeros((HEADS,), jnp.float32))
    unused, cells = lax.scan(advance, start, (query, keyed, valued, in_logs, running_log_total))
    centered = cells - lax.optimization_barrier(jnp.mean(cells, axis=-1, keepdims=True))
    normed = centered * lax.rsqrt(lax.optimization_barrier(jnp.mean(centered * centered, axis=-1, keepdims=True)) + EPSILON)
    normed = normed * head_norm_gain.reshape(HEADS, DV)[None, :, None, :]
    normed = normed.transpose(0, 2, 1, 3).reshape(TOKENS, HEADS * DV)
    gated = (normed * jax.nn.sigmoid(output_gate_logit.astype(jnp.float32))).astype(jnp.bfloat16)
    mixed = block_sum(gated, projection, N_TP)
    mixed = mixed * lax.rsqrt(lax.optimization_barrier(jnp.mean(mixed * mixed, axis=-1, keepdims=True)) + EPSILON) * cell_output_gain
    first_sum = (residual.astype(jnp.float32) + mixed).astype(jnp.bfloat16)
    first_wide = lax.optimization_barrier(first_sum).astype(jnp.float32)
    normed_rows = (first_wide * lax.rsqrt(lax.optimization_barrier(jnp.mean(first_wide * first_wide, axis=-1, keepdims=True)) + EPSILON) * mixer_input_gain).astype(jnp.bfloat16)
    gate_value = jnp.dot(normed_rows, mixer_gate_weight, preferred_element_type=jnp.float32)
    up_value = jnp.dot(normed_rows, mixer_up_weight, preferred_element_type=jnp.float32)
    activated = (jax.nn.silu(gate_value) * up_value).astype(jnp.bfloat16)
    channel_out = block_sum(activated, mixer_down_weight, N_TP)
    return (first_wide + 0.5 * channel_out).astype(jnp.bfloat16)
```

```python
import jax
import jax.numpy as jnp
from jax import lax
from jax.experimental import pallas as pl
from jax.experimental.pallas import tpu as pltpu
from jax.sharding import PartitionSpec as P

MESH = pl.DeviceIdType.MESH
F32, BF16 = jnp.float32, jnp.bfloat16
TOK, DQK, DV, WIDE, HID = 768, 128, 256, 2048, 640
NZ, NX, NY = 8, 4, 4
CUT = 768
ALL = 3 * HID
SCALE = DQK ** (-0.5)
EPSILON = 1e-06
LOW = -1e30
COPIES = 160


def dot(a, b):
    return lax.dot_general(a, b, (((1,), (0,)), ((), ())), preferred_element_type=F32)


def dot_nt(a, b):
    return lax.dot_general(a, b, (((1,), (1,)), ((), ())), preferred_element_type=F32)


def dot_tn(a, b):
    return lax.dot_general(a, b, (((0,), (0,)), ((), ())), preferred_element_type=F32)


class Wire:
    def __init__(self, send_sems, recv_sems):
        self.send_sems, self.recv_sems, self.open = send_sems, recv_sems, []

    def send(self, src, dst, to):
        k = len(self.open)
        copy = pltpu.make_async_remote_copy(
            src_ref=src,
            dst_ref=dst,
            send_sem=self.send_sems.at[k],
            recv_sem=self.recv_sems.at[k],
            device_id=to,
            device_id_type=MESH,
        )
        copy.start()
        self.open.append(copy)
        return copy


def rows_at(start, size, unit):
    return pl.ds(pl.multiple_of(start, unit), size)


def blocks(count, step):
    def run(i, carry):
        step(i)
        return carry

    lax.fori_loop(0, count, run, 0)


def layer(
    fg, ig, dec, hg, cg, mg,
    q_h, k_h, v_h, og_h, proj_h, res_h, wg_h, wu_h, wd_h,
    out,
    gates, rows_t, cols_t, acol, gcol, bcol,
    q, k, v, og, proj, res, w_all,
    num, den,
    st_own, st_row, ax_own, ax_row, sub, st_col, ax_sub, ax_col, st_out, st_prior,
    gated, part, part_sib, pair, ring, ring_sum,
    first, rows_n, hid, act,
    down, down_sib, pair2, ring2, ring2_sum,
    local_sems, send_sems, recv_sems,
):
    sp, tp = lax.axis_index("sp"), lax.axis_index("tp")
    z, x = sp // NX, lax.rem(sp, NX)
    y, c = tp // 2, lax.rem(tp, 2)
    wire = Wire(send_sems, recv_sems)

    def at(dz=0, dx=0, dy=0, flip=False):
        zz, xx = lax.rem(z + dz, NZ), lax.rem(x + dx, NX)
        yy, cc = lax.rem(y + dy, NY), (1 - c if flip else c)
        return (zz * NX + xx, yy * 2 + cc)

    sibling = at(flip=True)
    up_y, down_y = at(dy=1), at(dy=NY - 1)
    up_z, down_z = at(dz=1), at(dz=NZ - 1)
    up_x, down_x = at(dx=1), at(dx=NX - 1)

    own_w = rows_at(64 * sp, 64, 64)
    plan = [
        (wg_h, w_all.at[own_w, 0:HID]),
        (wu_h, w_all.at[own_w, HID : 2 * HID]),
        (wd_h, w_all.at[own_w, 2 * HID : 3 * HID]),
        (k_h, k),
        (v_h, v),
        (q_h, q),
        (og_h, og),
        (proj_h, proj),
        (res_h.at[rows_at(96 * tp, 96, 32), :], res),
    ]
    loads = [
        pltpu.make_async_copy(src, dst, local_sems.at[i]) for i, (src, dst) in enumerate(plan)
    ]
    for load in loads:
        load.start()
    load_w, (load_k, load_v, load_q, load_og, load_proj, load_res) = loads[:3], loads[3:]

    barrier = pltpu.get_barrier_semaphore()
    peers = [sibling, up_y, down_y]
    peers += [at(dz=o) for o in range(1, NZ)] + [at(dx=o) for o in range(1, NX)]
    for peer in peers:
        pl.semaphore_signal(barrier, inc=1, device_id=peer, device_id_type=MESH)

    lane = lax.broadcasted_iota(jnp.int32, (8, 128), 1)
    subl = lax.broadcasted_iota(jnp.int32, (8, 128), 0)

    def scan(value, op, identity):
        for shift in (1, 2, 4, 8, 16, 32, 64):
            moved = pltpu.roll(value, shift, axis=1)
            value = op(value, jnp.where(lane >= shift, moved, identity))
        total = jnp.broadcast_to(value[:, 127:128], (8, 128))
        for shift in (1, 2, 4):
            moved = pltpu.roll(total, shift, axis=0)
            total = op(total, jnp.where(subl >= shift, moved, identity))
        before = jnp.where(subl >= 1, pltpu.roll(total, 1, axis=0), identity)
        return op(value, before)

    for i, ref in enumerate((fg, ig, dec)):
        gates[i] = jnp.zeros((8, 128), F32)
        for r in range(6):
            gates[i, r : r + 1, :] = ref[0:1, 128 * r : 128 * (r + 1)]
    logit = gates[0]
    forget = jnp.minimum(logit, 0.0) - jnp.log1p(jnp.exp(-jnp.abs(logit))) + gates[2]
    total_log = scan(forget, jnp.add, 0.0)
    a_rows = gates[1] - total_log
    peak = scan(a_rows, jnp.maximum, LOW)
    decay_own = total_log[5:6, 127:128]
    a_max = peak[5:6, 127:128]
    rows_t[0:8, :] = a_rows
    rows_t[8:16, :] = peak
    rows_t[16:24, :] = total_log
    rows_t[24:128, :] = jnp.zeros((104, 128), F32)
    cols_t[...] = jnp.transpose(rows_t[...])
    for r in range(6):
        here = slice(128 * r, 128 * (r + 1))
        acol[here, :] = cols_t[:, r : r + 1]
        gcol[here, :] = cols_t[:, 8 + r : 9 + r]
        bcol[here, :] = cols_t[:, 16 + r : 17 + r]

    pl.semaphore_wait(barrier, len(peers))

    def piece(dz, dx, rows=64, skip=0):
        zz, xx = lax.rem(z + dz, NZ), lax.rem(x + dx, NX)
        return rows_at(64 * (NX * zz + xx) + skip, rows, 32)

    def run(dz, rows=256, skip=0):
        return rows_at(256 * lax.rem(z + dz, NZ) + skip, rows, 128)

    LEFT, RIGHT = slice(0, CUT), slice(CUT, ALL)

    def send_w(rows, cols, to):
        return wire.send(w_all.at[rows, cols], w_all.at[rows, cols], to)

    def a2(s):
        half = 128 if s == 4 else 256
        return (
            send_w(run(NZ + 1 - s, half), LEFT, up_z),
            send_w(run(s - 1, half, 256 - half), LEFT, down_z),
        )

    def b1(s):
        half = 32 if s == 4 else 64
        return (
            send_w(piece(NZ + 1 - s, 0, half), RIGHT, up_z),
            send_w(piece(s - 1, 0, half, 64 - half), RIGHT, down_z),
        )

    def b2(dz):
        return (send_w(piece(dz, 0), RIGHT, up_x), send_w(piece(dz, 0), RIGHT, down_x))

    def onward_up(dz):
        return send_w(piece(dz, NX - 1), RIGHT, up_x)

    def onward_down(dz):
        return send_w(piece(dz, 1), RIGHT, down_x)

    def landed(copies):
        for copy in copies:
            copy.wait_recv()

    for load in load_w:
        load.wait()
    A1 = [send_w(piece(0, 0), LEFT, at(dx=o)) for o in (1, 3, 2)]
    A2, B1, B2, ON = {}, {}, {}, {}
    B1[1] = b1(1)

    load_k.wait()
    load_v.wait()
    state = jnp.zeros((DQK, DV), F32)
    norm = jnp.zeros((1, DQK), F32)
    for i in range(3):
        here = slice(256 * i, 256 * (i + 1))
        lift = jnp.exp(acol[here, :] - a_max)
        keys = k[here, :]
        state = state + dot_tn(keys, (lift * v[here, :].astype(F32)).astype(BF16))
        norm = norm + jnp.sum(lift * keys.astype(F32), axis=0, keepdims=True)

    def wide(value):
        return jnp.broadcast_to(value, (1, 128))

    for j in range(NX):
        st_own[j] = state[32 * j : 32 * (j + 1), :].astype(BF16)
    ax_own[...] = jnp.concatenate(
        [norm, wide(decay_own), wide(decay_own + a_max), jnp.zeros((5, 128), F32)], axis=0
    )
    S1 = []
    for o in range(1, NX):
        S1.append(wire.send(st_own.at[lax.rem(x + o, NX)], st_row.at[x], at(dx=o)))
        S1.append(wire.send(ax_own, ax_row.at[x], at(dx=o)))
    st_row[x] = st_own[x]
    ax_row[x] = ax_own[...]
    B2[0] = b2(0)

    load_q.wait()
    diagonal = lax.broadcasted_iota(jnp.int32, (256, 256), 0) >= lax.broadcasted_iota(
        jnp.int32, (256, 256), 1
    )

    def attend(i):
        here = slice(256 * i, 256 * (i + 1))
        queries = q[here, :]
        top = gcol[here, :]
        over = jnp.zeros((256, DV), F32)
        under = jnp.zeros((256, 1), F32)
        for j in range(i + 1):
            there = slice(256 * j, 256 * (j + 1))
            a_line = jnp.concatenate(
                [rows_t[2 * j : 2 * j + 1, :], rows_t[2 * j + 1 : 2 * j + 2, :]], axis=1
            )
            power = a_line - top
            if i == j:
                power = jnp.where(diagonal, power, LOW)
            weight = jnp.exp(power) * (dot_nt(queries, k[there, :]) * SCALE)
            under = under + jnp.sum(weight, axis=1, keepdims=True)
            over = over + dot(weight.astype(BF16), v[there, :])
        num[here, :] = over
        den[here, :] = under

    attend(0)
    landed(A1)
    A2[1] = a2(1)

    landed(S1)
    decay = [ax_row[i, 1:2, :] for i in range(NX)]
    peaks = [ax_row[i, 2:3, :] for i in range(NX)]
    norms = [ax_row[i, 0:1, :] for i in range(NX)]

    def between(i, j):
        total = jnp.zeros((1, 128), F32)
        for m in range(i + 1, j):
            total = total + decay[m]
        return total

    tops = [peaks[i] + between(i, NX) for i in range(NX)]
    row_peak = jnp.maximum(jnp.maximum(tops[0], tops[1]), jnp.maximum(tops[2], tops[3]))
    gains = [jnp.exp(top - row_peak) for top in tops]
    row_state = sum(gains[i][:, 0:1] * st_row[i].astype(F32) for i in range(NX))
    row_norm = sum(gains[i] * norms[i] for i in range(NX))
    sub[...] = row_state.astype(BF16)
    ax_sub[...] = jnp.concatenate(
        [row_norm, between(-1, NX), row_peak, jnp.zeros((5, 128), F32)], axis=0
    )
    S2 = []
    for o in (4, 3, 5, 2, 6, 1, 7):
        S2.append(wire.send(sub, st_col.at[z], at(dz=o)))
        S2.append(wire.send(ax_sub, ax_col.at[z], at(dz=o)))
    st_col[z] = sub[...]
    ax_col[z] = ax_sub[...]

    landed(B1[1])
    B1[2] = b1(2)
    B2[1], B2[7] = b2(1), b2(NZ - 1)
    attend(1)
    attend(2)

    landed(S2)
    col_peak = jnp.full((1, 128), LOW, F32)
    col_decay = jnp.zeros((1, 128), F32)
    col_norm = jnp.zeros((1, 128), F32)
    col_state = jnp.zeros((32, DV), F32)
    for zz in range(NZ - 1):
        passed = zz < z
        late_decay, late_peak = ax_col[zz, 1:2, :], ax_col[zz, 2:3, :]
        joined = jnp.maximum(late_decay + col_peak, late_peak)
        f1 = jnp.where(passed, jnp.exp(late_decay + col_peak - joined), 1.0)
        f2 = jnp.where(passed, jnp.exp(late_peak - joined), 0.0)
        col_state = f1[:, 0:1] * col_state + f2[:, 0:1] * st_col[zz].astype(F32)
        col_norm = f1 * col_norm + f2 * ax_col[zz, 0:1, :]
        col_decay = jnp.where(passed, col_decay + late_decay, col_decay)
        col_peak = jnp.where(passed, joined, col_peak)

    start = jnp.zeros((1, 128), F32)
    prior_norm = jnp.zeros((1, 128), F32)
    for t in range(NX):
        row_decay = between(-1, t)
        highest = row_decay + jnp.maximum(col_peak, col_decay)
        for i in range(t):
            highest = jnp.maximum(highest, peaks[i] + between(i, t))
        f0 = jnp.exp(row_decay + col_peak - highest)
        joint, joint_norm = f0[:, 0:1] * col_state, f0 * col_norm
        for i in range(t):
            f = jnp.exp(peaks[i] + between(i, t) - highest)
            joint = joint + f[:, 0:1] * st_row[i].astype(F32)
            joint_norm = joint_norm + f * norms[i]
        st_out[t] = joint.astype(BF16)
        start = jnp.where(x == t, highest, start)
        prior_norm = jnp.where(x == t, joint_norm, prior_norm)
    S3 = [
        wire.send(st_out.at[lax.rem(x + o, NX)], st_prior.at[x], at(dx=o)) for o in range(1, NX)
    ]
    st_prior[x] = st_out[x]
    landed(A2[1])
    A2[2] = a2(2)
    landed(B2[0])
    ON[0] = onward_up(0)
    load_og.wait()
    load_proj.wait()
    load_res.wait()

    landed(S3)
    prior = st_prior[...].reshape(DQK, DV)
    start = start[:, 0:1]

    def finish_cell(i):
        here = slice(256 * i, 256 * (i + 1))
        own_top = gcol[here, :]
        top = jnp.maximum(own_top, start)
        keep = jnp.exp(own_top - top)
        carry = jnp.exp(start - top) * SCALE
        queries = q[here, :]
        over = keep * num[here, :] + carry * dot(queries, prior)
        under = keep * den[here, :] + carry * jnp.sum(
            queries.astype(F32) * prior_norm, axis=1, keepdims=True
        )
        floor = jnp.exp(-(bcol[here, :] + top))
        cell = over / jnp.maximum(jnp.abs(under), floor)
        centred = cell - jnp.mean(cell, axis=1, keepdims=True)
        spread = jnp.mean(centred * centred, axis=1, keepdims=True)
        normed = centred * lax.rsqrt(spread + EPSILON) * hg[...]
        gated[here, :] = (normed * jax.nn.sigmoid(og[here, :].astype(F32))).astype(BF16)

    for i in range(3):
        finish_cell(i)
    landed(B1[2])
    B1[3] = b1(3)
    B2[2], B2[6] = b2(2), b2(NZ - 2)

    def project(o):
        yy = lax.rem(y + o, NY)
        here = rows_at(192 * yy, 192, 64)
        left = gated[here, :]
        for n in range(8):
            cols = slice(256 * n, 256 * (n + 1))
            part[here, cols] = dot(left, proj[:, cols]).astype(BF16)
        theirs = rows_at(96 * (2 * yy + 1 - c), 96, 32)
        return wire.send(part.at[theirs, :], part_sib.at[o], sibling)

    def pair_up(o):
        yy = lax.rem(y + o, NY)

        def step(i):
            mine = rows_at(96 * (2 * yy + c) + 16 * i, 16, 16)
            here = rows_at(16 * i, 16, 16)
            total = part[mine, :].astype(F32) + part_sib[o, here, :].astype(F32)
            pair[o, here, :] = total.astype(BF16)

        blocks(6, step)

    H0, H1 = slice(0, 48), slice(48, 96)
    D = {}
    D[2] = project(2)
    D[1] = project(1)
    landed([D[2]])
    pair_up(2)
    M1 = wire.send(pair.at[2, H0, :], ring.at[0], up_y)
    M1b = wire.send(pair.at[2, H1, :], ring.at[1], down_y)
    D[3] = project(3)
    landed([D[1]])
    pair_up(1)
    M2 = wire.send(pair.at[1, H1, :], ring.at[2], up_y)
    D[0] = project(0)
    landed([D[3]])
    pair_up(3)
    M2b = wire.send(pair.at[3, H0, :], ring.at[3], down_y)

    landed(A2[2])
    A2[3] = a2(3)
    landed(B2[1] + B2[7])
    ON[7] = onward_up(NZ - 1)
    ON[1] = onward_down(1)

    landed([D[0]])
    pair_up(0)

    def ring_add(o, skip, slot, into):
        def step(i):
            here = rows_at(16 * i, 16, 16)
            there = rows_at(16 * i + skip, 16, 16)
            total = pair[o, there, :].astype(F32) + ring[slot, here, :].astype(F32)
            ring_sum[into, here, :] = total.astype(BF16)

        blocks(3, step)

    landed([M1])
    ring_add(1, 0, 0, 0)
    M3 = wire.send(ring_sum.at[0], ring.at[4], up_y)
    landed([M1b])
    ring_add(3, 48, 1, 1)
    M3b = wire.send(ring_sum.at[1], ring.at[5], down_y)

    landed(B1[3])
    B1[4] = b1(4)
    B2[3], B2[5] = b2(3), b2(NZ - 3)
    landed(B2[2] + B2[6])
    ON[6] = onward_up(NZ - 2)
    ON[2] = onward_down(2)

    own_first = 96 * tp

    def finish_mix(skip, one, two):
        def step(i):
            here = rows_at(16 * i, 16, 16)
            there = rows_at(16 * i + skip, 16, 16)
            mix = (
                pair[0, there, :].astype(F32)
                + ring[one, here, :].astype(F32)
                + ring[two, here, :].astype(F32)
            )
            scale = lax.rsqrt(jnp.mean(mix * mix, axis=1, keepdims=True) + EPSILON)
            total = res[there, :].astype(F32) + mix * scale * cg[...]
            first[rows_at(own_first + skip + 16 * i, 16, 16), :] = total.astype(BF16)

        blocks(3, step)

    def first_rows(dy, half, cc):
        return rows_at(96 * (2 * lax.rem(y + dy, NY) + cc) + 48 * half, 48, 16)

    def share(dy, half, to):
        rows = first_rows(dy, half, c)
        return wire.send(first.at[rows, :], first.at[rows, :], to)

    landed([M3, M2b])
    finish_mix(0, 4, 3)
    N1, N2b, E0 = share(0, 0, up_y), share(0, 0, down_y), share(0, 0, sibling)
    landed([M2, M3b])
    finish_mix(48, 2, 5)
    N2, N1b, E1 = share(0, 1, up_y), share(0, 1, down_y), share(0, 1, sibling)

    landed(A2[3])
    A2[4] = a2(4)
    landed(B1[4])
    B2[4] = b2(4)
    landed(B2[3] + B2[5])
    ON[5] = onward_up(NZ - 3)
    ON[3] = onward_down(3)

    landed([N1])
    N3, E2 = share(3, 0, up_y), share(3, 0, sibling)
    landed([N1b])
    N3b, E3 = share(1, 1, down_y), share(1, 1, sibling)

    landed(B2[4])
    ON[4] = onward_down(4)
    landed([N2])
    E4 = share(3, 1, sibling)
    landed([N2b])
    E5 = share(1, 0, sibling)
    landed(A2[4])
    for s in range(NZ):
        landed([ON[s]])

    def mixer(o):
        yy = lax.rem(y + o, NY)

        def normalise(i):
            rows = first[rows_at(192 * yy + 16 * i, 16, 16), :].astype(F32)
            scale = lax.rsqrt(jnp.mean(rows * rows, axis=1, keepdims=True) + EPSILON)
            rows_n[rows_at(16 * i, 16, 16), :] = (rows * scale * mg[...]).astype(BF16)

        blocks(12, normalise)

        def widen(i):
            cols = pl.ds(pl.multiple_of(256 * i, 256), 256)
            hid[:, cols] = dot(rows_n[...], w_all[:, cols])

        blocks(5, widen)

        def activate(i):
            here = rows_at(16 * i, 16, 16)
            gate, value = hid[here, 0:HID], hid[here, HID : 2 * HID]
            act[here, :] = (gate * jax.nn.sigmoid(gate) * value).astype(BF16)

        blocks(12, activate)

        def narrow(cc):
            def step(i):
                rows = rows_at(256 * (2 * i + cc), 256, 256)
                total = dot_nt(act[...], w_all[rows, 2 * HID : 3 * HID])
                down[o, cc, i] = total.astype(BF16)

            blocks(4, step)

        narrow(1 - c)
        theirs = wire.send(down.at[o, 1 - c], down_sib.at[o], sibling)
        narrow(c)
        return theirs

    G, G1, G1b, G2, G2b, G3, G3b = {}, {}, {}, {}, {}, {}, {}

    def group(o):
        return lax.rem(y + o, NY)

    L0, L1 = slice(0, 96), slice(96, 192)

    def spread_out(o):
        landed([G[o]])

        def add(p):
            yy = lax.rem(y + p, NY)

            def step(i):
                here = rows_at(32 * i, 32, 32)
                total = down[o, c, yy, here, :].astype(F32) + down_sib[o, yy, here, :].astype(F32)
                pair2[o, p, here, :] = total.astype(BF16)

            blocks(6, step)

        add(2)
        G1[o] = wire.send(pair2.at[o, 2, L0, :], ring2.at[group(o), 0], up_y)
        G1b[o] = wire.send(pair2.at[o, 2, L1, :], ring2.at[group(o), 1], down_y)
        add(1)
        G2[o] = wire.send(pair2.at[o, 1, L1, :], ring2.at[group(o), 2], up_y)
        add(3)
        G2b[o] = wire.send(pair2.at[o, 3, L0, :], ring2.at[group(o), 3], down_y)
        add(0)

    def ring2_add(o, p, skip, slot, into):
        def step(i):
            here = rows_at(32 * i, 32, 32)
            there = rows_at(32 * i + skip, 32, 32)
            total = pair2[o, p, there, :].astype(F32) + ring2[group(o), slot, here, :].astype(F32)
            ring2_sum[o, into, here, :] = total.astype(BF16)

        blocks(3, step)

    def pass_up(o):
        landed([G1[(o + 1) % NY]])
        ring2_add(o, 1, 0, 0, 0)
        G3[o] = wire.send(ring2_sum.at[o, 0], ring2.at[group(o), 4], up_y)

    def pass_down(o):
        landed([G1b[(o + 3) % NY]])
        ring2_add(o, 3, 96, 1, 1)
        G3b[o] = wire.send(ring2_sum.at[o, 1], ring2.at[group(o), 5], down_y)

    landed([E0, E1])
    G[0] = mixer(0)
    spread_out(0)
    landed([N3])
    E6 = share(2, 0, sibling)
    landed([N3b])
    E7 = share(2, 1, sibling)
    landed([E3, E5])
    G[1] = mixer(1)
    spread_out(1)
    landed([E2, E4])
    G[3] = mixer(3)
    spread_out(3)
    landed([E6, E7])
    G[2] = mixer(2)
    spread_out(2)
    for o_up, o_down in ((3, 1), (0, 2), (2, 0), (1, 3)):
        pass_up(o_up)
        pass_down(o_down)

    own_cols = pl.ds(pl.multiple_of(DV * tp, DV), DV)

    def finish(o, skip, one, two):
        def step(i):
            here = rows_at(32 * i, 32, 32)
            there = rows_at(32 * i + skip, 32, 32)
            rows = rows_at(192 * group(o) + skip + 32 * i, 32, 32)
            total = (
                pair2[o, 0, there, :].astype(F32)
                + ring2[group(o), one, here, :].astype(F32)
                + ring2[group(o), two, here, :].astype(F32)
            )
            out[rows, :] = (first[rows, own_cols].astype(F32) + 0.5 * total).astype(BF16)

        blocks(3, step)

    for o in (0, 3, 1, 2):
        landed([G3[(o + 1) % NY], G2b[(o + 3) % NY]])
        finish(o, 0, 4, 3)
        landed([G2[(o + 1) % NY], G3b[(o + 3) % NY]])
        finish(o, 96, 2, 5)

    for copy in wire.open:
        copy.wait_send()


def body(
    residual, query, key, value, gate_logit, in_gate, forget_logit, decay,
    head_gain, projection, cell_gain, mixer_gain, gate_w, up_w, down_w,
):
    line = lambda a: a.reshape(1, -1)
    vmem = lambda *dims: pltpu.VMEM(dims, BF16)
    wide = lambda *dims: pltpu.VMEM(dims, F32)
    scratch = [
        wide(3, 8, 128), wide(128, 128), wide(128, 128),
        wide(TOK, 1), wide(TOK, 1), wide(TOK, 1),
        vmem(TOK, DQK), vmem(TOK, DQK), vmem(TOK, DV), vmem(TOK, DV),
        vmem(DV, WIDE), vmem(96, WIDE), vmem(WIDE, ALL),
        wide(TOK, DV), wide(TOK, 1),
        vmem(NX, 32, DV), vmem(NX, 32, DV), wide(8, 128), wide(NX, 8, 128),
        vmem(32, DV), vmem(NZ, 32, DV), wide(8, 128), wide(NZ, 8, 128),
        vmem(NX, 32, DV), vmem(NX, 32, DV),
        vmem(TOK, DV), vmem(TOK, WIDE), vmem(NY, 96, WIDE), vmem(NY, 96, WIDE),
        vmem(6, 48, WIDE), vmem(2, 48, WIDE),
        vmem(TOK, WIDE), vmem(192, WIDE), wide(192, 2 * HID), vmem(192, HID),
        vmem(NY, 2, NY, 192, DV), vmem(NY, NY, 192, DV), vmem(NY, NY, 192, DV),
        vmem(NY, 6, 96, DV), vmem(NY, 2, 96, DV),
        pltpu.SemaphoreType.DMA((9,)),
        pltpu.SemaphoreType.DMA((COPIES,)),
        pltpu.SemaphoreType.DMA((COPIES,)),
    ]
    in_vmem = pl.BlockSpec(memory_space=pltpu.VMEM)
    in_hbm = pl.BlockSpec(memory_space=pltpu.HBM)
    return pl.pallas_call(
        layer,
        out_shape=jax.ShapeDtypeStruct((TOK, DV), BF16),
        in_specs=[in_vmem] * 6 + [in_hbm] * 9,
        out_specs=in_vmem,
        scratch_shapes=scratch,
        compiler_params=pltpu.CompilerParams(
            collective_id=0, has_side_effects=True, vmem_limit_bytes=60 * 1024 * 1024
        ),
    )(
        line(forget_logit), line(in_gate), line(decay),
        line(head_gain), line(cell_gain), line(mixer_gain),
        query, key, value, gate_logit, projection, residual, gate_w, up_w, down_w.T,
    )


def solution(mesh):
    placed = (
        P("sp", None), P("sp", "tp"), P("sp", "tp"), P("sp", "tp"), P("sp", "tp"),
        P("sp", "tp"), P("sp", "tp"), P("sp", "tp"),
        P("tp"), P("tp", None), P(), P(),
        P("sp", "tp"), P("sp", "tp"), P("tp", "sp"),
    )
    return jax.shard_map(body, mesh=mesh, in_specs=placed, out_specs=P("sp", "tp"), check_vma=False)
```
